32 devices in a mesh: grp: 2 (over x), ep: 16 (over z, y, core).
Axes of the slice: x: 2, y: 2, z: 4, core: 2. Of those that a mesh axis runs over, the one named last changes fastest.
Arguments:
- tokens: bfloat16 [512, 2048], P(('grp', 'ep')), parts along dimension 0, may hold values from -6 to 6
- attn_gain: float32 [2048], replicated, may hold values from 0.1 to 1.9
- w_query: bfloat16 [2048, 1024], replicated, may hold values from -0.125 to 0.125
- w_key: bfloat16 [2048, 128], replicated, may hold values from -0.125 to 0.125
- w_value: bfloat16 [2048, 128], replicated, may hold values from -0.125 to 0.125
- w_forget: bfloat16 [2048, 2], replicated, may hold values from -0.125 to 0.125
- forget_bias: float32 [2], replicated, may hold values from -3 to 1
- w_attn_out: bfloat16 [1024, 2048], replicated, may hold values from -0.1875 to 0.1875
- cache_keys: bfloat16 [512, 1024, 128], P(('grp', 'ep')), parts along dimension 0, may hold values from -640 to 640
- cache_values: bfloat16 [512, 1024, 128], P(('grp', 'ep')), parts along dimension 0, may hold values from -6 to 6
- cache_logsum: float32 [512, 2, 1024], P(('grp', 'ep')), parts along dimension 0, may hold values from -100 to 0, as said below
- lengths: int32 [512], P(('grp', 'ep')), parts along dimension 0, may hold values from 1 to 1024, as said below
- ffn_gain: float32 [2048], replicated, may hold values from 0.1 to 1.9
- branch_gate: float32 [2048], replicated, may hold values from -0.125 to 0.125
- dense_gate: bfloat16 [2048, 4096], P(None, 'ep'), may hold values from -0.125 to 0.125
- dense_up: bfloat16 [2048, 4096], P(None, 'ep'), may hold values from -0.125 to 0.125
- dense_down: bfloat16 [4096, 2048], P('ep'), may hold values from -0.09375 to 0.09375
- expert_gate: bfloat16 [16, 2048, 512], P('ep'), may hold values from -0.125 to 0.125
- expert_up: bfloat16 [16, 2048, 512], P('ep'), may hold values from -0.125 to 0.125
- expert_down: bfloat16 [16, 512, 2048], P('ep'), may hold values from -0.25 to 0.25
- routes: int32 [512, 4], P(('grp', 'ep')), parts along dimension 0, may hold values from 0 to 15, all different within a row; in each aligned block of 16 rows (0 to 15, 16 to 31, ...) at most 8 rows name the same one
- route_weights: float32 [512, 4], P(('grp', 'ep')), parts along dimension 0, may hold values from 0.2 to 1
Outputs:
- output_rows: bfloat16 [512, 2048], P(('grp', 'ep')), parts along dimension 0
The draws below stay inside these ranges and needn't reach their ends.
There are 2 independent parts, one for each index of `grp`. The reference program is written for one: setup_inputs(seed, part) draws one part's arguments, and reference() takes and returns one part's arrays. A program takes and returns all parts, laid end to end along the dimension named above; an argument that names none is the same for every part. Nothing has to cross between parts.
Inputs may be any that keep to these rules, and one draw needn't show every extreme that they name: `lengths`: each aligned block of 16 sequences holds one with 1024 valid positions; every length is at least 128. `routes`: a row's 4 experts differ; among the rows of one device no expert is named more than 8 times. `cache_logsum`: non-increasing along positions.
All inputs are finite; a program needn't handle non-finite values.
Results may differ from the reference program's by a relative error of at most 0.012.
The reference program's roundings to bfloat16 on the way count: a program that leaves them out, or rounds other values in their place, can miss the bound.
Values may be sent and summed in bfloat16 or wider, within the bound.
A program may use at most 128 MiB of HBM per device.

```python
import math
import jax
import jax.numpy as jnp
import numpy as np
from jax import lax

D = 2048
HEADS = 16
HD = 64
KEY_VALUE_HEADS = 2
EH = 512
DENSE_FF = 4096
TOPK = 4
CACHE_POSITIONS = 1024
SEQ_DEV = 16
SEQUENCE_TOTAL = 256
EXPERTS = 16
CAP = 8
N_EP = 16


def draw_lengths(key, part):
    first_key, second_key = jax.random.split(jax.random.fold_in(key, 11))
    drawn = jax.random.randint(first_key, (SEQUENCE_TOTAL,), CACHE_POSITIONS // 8, CACHE_POSITIONS + 1)
    chosen = jax.random.randint(second_key, (SEQUENCE_TOTAL // SEQ_DEV,), 0, SEQ_DEV)
    ordinal = jnp.arange(SEQUENCE_TOTAL, dtype=jnp.int32)
    filled = ordinal % SEQ_DEV == jnp.repeat(chosen, SEQ_DEV)
    return jnp.where(filled, CACHE_POSITIONS, drawn).astype(jnp.int32)


def draw_cache_keys(key, part):
    random_subkeys = jax.random.split(jax.random.fold_in(key, 21), 1)
    row_width = KEY_VALUE_HEADS * HD
    drawn = jax.random.truncated_normal(random_subkeys[0], -6.0, 6.0, (SEQUENCE_TOTAL, CACHE_POSITIONS, row_width), jnp.float32)
    return drawn.astype(jnp.bfloat16)


def draw_cache_logsum(key, part):
    random_subkeys = jax.random.split(jax.random.fold_in(key, 31), 7)
    head_shape = (SEQUENCE_TOTAL, KEY_VALUE_HEADS, 1)
    slow_share = 0.5
    slow_flag = jax.random.uniform(random_subkeys[0], head_shape) < slow_share
    slow_rate = jnp.exp(jax.random.uniform(random_subkeys[1], head_shape, jnp.float32, math.log(0.1), math.log(0.6))) / CACHE_POSITIONS
    fast_rate = jnp.exp(jax.random.uniform(random_subkeys[2], head_shape, jnp.float32, math.log(0.01), math.log(1.0 / 30.0)))
    selected_rate = jnp.where(slow_flag, slow_rate, fast_rate)
    group_member = jnp.exp(jax.random.uniform(random_subkeys[3], (SEQUENCE_TOTAL, 1, 1), jnp.float32, math.log(0.7), math.log(1.4)))
    jaggedness = jax.random.uniform(random_subkeys[4], (SEQUENCE_TOTAL, KEY_VALUE_HEADS, CACHE_POSITIONS), jnp.float32, 0.3, 1.7)
    spike_locations = jax.random.randint(random_subkeys[5], (SEQUENCE_TOTAL, KEY_VALUE_HEADS, 2), 0, CACHE_POSITIONS)
    spike_penalty = jax.random.uniform(random_subkeys[6], (SEQUENCE_TOTAL, KEY_VALUE_HEADS, 2), jnp.float32, 0.22, 0.5)
    cache_position = lax.broadcasted_iota(jnp.int32, (SEQUENCE_TOTAL, KEY_VALUE_HEADS, 2, CACHE_POSITIONS), 3)
    spike_events = jnp.sum(jnp.where(cache_position == spike_locations[..., None], spike_penalty[..., None], 0.0), axis=2)
    step_increments = -selected_rate * group_member * jaggedness - jnp.where(slow_flag, spike_events, 0.0)
    return jnp.cumsum(step_increments, axis=2)


def steps_of(own_key, shape, shards, smallest, largest):
    gain = 1.0
    for axis_at, parts in shards:
        heights = jax.random.uniform(jax.random.fold_in(jax.random.fold_in(own_key, 6), axis_at), (parts,), jnp.float32, smallest / len(shards), largest / len(shards))
        gain = gain * jnp.repeat(jnp.exp(heights), shape[axis_at] // parts).reshape((-1,) + (1,) * (len(shape) - 1 - axis_at))
    return gain


def assign_block(rng, own, number, rows, amount, top, bound, slope):
    order = jax.random.permutation(rng, amount)
    heavy_load, ordinary = load_shares(amount, rows * top, bound, slope, True), load_shares(amount, rows * top, bound, slope, False)
    places = jnp.arange(amount)

    def named(tallies, rotation):
        used = int((tallies > 0).sum())
        fixed = max(1, used // 4)
        passed = fixed + (places - fixed + rotation * (used - fixed)) % max(1, amount - fixed)
        return jnp.zeros((amount,), jnp.int32).at[order[jnp.where(places < fixed, places, passed)]].set(jnp.asarray(tallies, jnp.int32))

    tallies = jnp.where(number % 4 == 0, named(heavy_load, number // 4), named(ordinary, number - number // 4 - 1))
    mixed = jax.random.permutation(jax.random.fold_in(own, 3), amount)
    source_of, sink = mixed[0:amount // 2 * 2:2], mixed[1:amount // 2 * 2:2]
    margin = jnp.minimum(tallies[source_of] - 1, bound - tallies[sink]) // 2
    margin = jnp.where((source_of == order[0]) | (sink == order[0]) | (tallies[sink] == 0), 0, jnp.maximum(margin, 0))
    passed = jax.random.randint(jax.random.fold_in(own, 4), (amount // 2,), 0, 1 << 20) % (margin + 1)
    tallies = tallies.at[source_of].add(-passed).at[sink].add(passed)
    labels = jnp.searchsorted(jnp.cumsum(tallies), jnp.arange(rows * top), side="right").astype(jnp.int32)
    listing = labels.reshape(top, rows).T
    listing = listing[jax.random.permutation(jax.random.fold_in(own, 1), rows)]
    rotation = jax.random.randint(jax.random.fold_in(own, 2), (rows, 1), 0, top)
    return jnp.take_along_axis(listing, (jnp.arange(top)[None, :] + rotation) % top, axis=1)


def load_shares(amount, total, most, skew, full):
    loads = [(1 << 20) // math.isqrt(rank ** skew) + 1 for rank in range(1, amount + 1)]
    largest = most if full else min(most, max(-(-total // amount), total * loads[0] // sum(loads)))
    least = 1 if total - largest >= amount - 1 else 0
    counts, rest = [largest] + [least] * (amount - 1), total - largest - least * (amount - 1)
    while rest > 0:
        candidates = [i for i in range(1, amount) if counts[i] < largest] or [i for i in range(1, amount) if counts[i] < most]
        whole, left = sum([loads[i] for i in candidates]), rest
        for i in candidates:
            more = min(most - counts[i], max(1, left * loads[i] // whole), rest)
            counts[i] = counts[i] + more
            rest = rest - more
    return np.array(counts)


def bell_draw(rng, extent, spread, bound, shards=(), kind=jnp.bfloat16):
    values = spread * jax.random.normal(rng, extent, jnp.float32)
    if shards:
        values = values * steps_of(rng, extent, shards, -0.22, 0.18)
    return jnp.clip(values, -bound, bound).astype(kind)


def setup_inputs(seed: int = 0, part: int = 0) -> dict:
    seeds = jax.random.split(jax.random.key(seed), 23)
    part_keys = jax.random.split(jax.random.fold_in(seeds[22], part), 23)
    tokens = bell_draw(part_keys[0], (SEQUENCE_TOTAL, D), 1.0, 6.0, ((0, 16),))
    attn_gain = jnp.clip(1.0 + 0.18 * jax.random.normal(seeds[1], (D,), jnp.float32), 0.1, 1.9)
    w_query = bell_draw(seeds[2], (D, HEADS * HD), D ** -0.5, 0.125)
    w_key = bell_draw(seeds[3], (D, KEY_VALUE_HEADS * HD), D ** -0.5, 0.125)
    w_value = bell_draw(seeds[4], (D, KEY_VALUE_HEADS * HD), D ** -0.5, 0.125)
    w_forget = bell_draw(seeds[5], (D, KEY_VALUE_HEADS), D ** -0.5, 0.125)
    forget_bias = jnp.clip(jax.random.uniform(seeds[6], (KEY_VALUE_HEADS,), jnp.float32, -3.0, 1.0), -3.0, 1.0)
    w_attn_out = bell_draw(seeds[7], (HEADS * HD, D), (HEADS * HD) ** -0.5, 0.1875)
    cache_keys = draw_cache_keys(jax.random.fold_in(jax.random.fold_in(seeds[22], part), 71), part)
    cache_values = bell_draw(part_keys[9], (SEQUENCE_TOTAL, CACHE_POSITIONS, KEY_VALUE_HEADS * HD), 1.0, 6.0, ((0, 16),))
    cache_logsum = draw_cache_logsum(jax.random.fold_in(jax.random.fold_in(seeds[22], part), 71), part)
    lengths = draw_lengths(jax.random.fold_in(jax.random.fold_in(seeds[22], part), 71), part)
    ffn_gain = jnp.clip(1.0 + 0.18 * jax.random.normal(seeds[12], (D,), jnp.float32), 0.1, 1.9)
    branch_gate = bell_draw(seeds[13], (D,), D ** -0.5, 0.125, (), jnp.float32)
    dense_gate = bell_draw(seeds[14], (D, DENSE_FF), D ** -0.5, 0.125, ((1, 16),))
    dense_up = bell_draw(seeds[15], (D, DENSE_FF), D ** -0.5, 0.125, ((1, 16),))
    dense_down = bell_draw(seeds[16], (DENSE_FF, D), DENSE_FF ** -0.5, 0.09375, ((0, 16),))
    expert_gate = bell_draw(seeds[17], (EXPERTS, D, EH), D ** -0.5, 0.125, ((0, 16),))
    expert_up = bell_draw(seeds[18], (EXPERTS, D, EH), D ** -0.5, 0.125, ((0, 16),))
    expert_down = bell_draw(seeds[19], (EXPERTS, EH, D), EH ** -0.5, 0.25, ((0, 16),))
    routes_keys = jax.random.split(jax.random.fold_in(part_keys[20], 1), SEQUENCE_TOTAL // SEQ_DEV)
    routes_turns = jax.random.permutation(jax.random.fold_in(part_keys[20], 3), SEQUENCE_TOTAL // SEQ_DEV)
    routes = jax.vmap(lambda own, number: assign_block(jax.random.fold_in(part_keys[20], 2), own, number, SEQ_DEV, EXPERTS, TOPK, CAP, 2))(routes_keys, routes_turns).reshape((SEQUENCE_TOTAL, TOPK))
    route_weights = jnp.clip(0.2 + 0.8 * jax.random.uniform(part_keys[21], (SEQUENCE_TOTAL, TOPK), jnp.float32) ** steps_of(part_keys[21], (SEQUENCE_TOTAL, TOPK), ((0, 16),), -0.2, 0.2), 0.2, 1.0)
    return dict(tokens=tokens, attn_gain=attn_gain, w_query=w_query, w_key=w_key, w_value=w_value, w_forget=w_forget, forget_bias=forget_bias, w_attn_out=w_attn_out, cache_keys=cache_keys, cache_values=cache_values, cache_logsum=cache_logsum, lengths=lengths, ffn_gain=ffn_gain, branch_gate=branch_gate, dense_gate=dense_gate, dense_up=dense_up, dense_down=dense_down, expert_gate=expert_gate, expert_up=expert_up, expert_down=expert_down, routes=routes, route_weights=route_weights)


EPSILON = 1e-06

def norm_rows(inputs, gain_vec):
    widened = inputs.astype(jnp.float32)
    scaled = widened * lax.rsqrt(lax.optimization_barrier(jnp.mean(widened * widened, axis=-1, keepdims=True)) + EPSILON)
    return (scaled * gain_vec).astype(jnp.bfloat16)

def swiglu(row_block, w_first, w_second):
    gate_part = jnp.dot(row_block, w_first, preferred_element_type=jnp.float32)
    up_part = jnp.dot(row_block, w_second, preferred_element_type=jnp.float32)
    return (jax.nn.silu(gate_part) * up_part).astype(jnp.bfloat16)

def expert_rows(row_block, w_gate, w_up, w_down):
    middle = swiglu(row_block, w_gate, w_up)
    return jnp.dot(middle, w_down, preferred_element_type=jnp.float32).astype(jnp.bfloat16)

def reference(tokens, attn_gain, w_query, w_key, w_value, w_forget, forget_bias, w_attn_out, cache_keys, cache_values, cache_logsum, lengths, ffn_gain, branch_gate, dense_gate, dense_up, dense_down, expert_gate, expert_up, expert_down, routes, route_weights):
    group_size = HEADS // KEY_VALUE_HEADS
    scaling = 1.0 / math.sqrt(HD)
    normed = norm_rows(tokens, attn_gain)
    queries = jnp.dot(normed, w_query, preferred_element_type=jnp.float32).astype(jnp.bfloat16)
    new_keys = jnp.dot(normed, w_key, preferred_element_type=jnp.float32).astype(jnp.bfloat16)
    new_values = jnp.dot(normed, w_value, preferred_element_type=jnp.float32).astype(jnp.bfloat16)
    log_gate = jax.nn.log_sigmoid(jnp.dot(normed, w_forget, preferred_element_type=jnp.float32) + forget_bias)
    positions = lax.broadcasted_iota(jnp.int32, (SEQUENCE_TOTAL, KEY_VALUE_HEADS, CACHE_POSITIONS), 2)
    latest = lax.optimization_barrier(jnp.sum(jnp.where(positions == lengths[:, None, None] - 1, cache_logsum, 0.0), axis=2))
    offsets = (latest + log_gate)[:, :, None] - cache_logsum
    usable = positions < lengths[:, None, None]
    query_heads = queries.reshape(SEQUENCE_TOTAL, KEY_VALUE_HEADS, group_size, HD).astype(jnp.float32)
    key_heads = cache_keys.reshape(SEQUENCE_TOTAL, CACHE_POSITIONS, KEY_VALUE_HEADS, HD).astype(jnp.float32)
    value_heads = cache_values.reshape(SEQUENCE_TOTAL, CACHE_POSITIONS, KEY_VALUE_HEADS, HD).astype(jnp.float32)
    scores = jnp.einsum('bgrd,blgd->bgrl', query_heads, key_heads) * scaling
    scores = jnp.where(usable[:, :, None, :], scores + offsets[:, :, None, :], -jnp.inf)
    self_score = jnp.einsum('bgrd,bgd->bgr', query_heads, new_keys.reshape(SEQUENCE_TOTAL, KEY_VALUE_HEADS, HD).astype(jnp.float32)) * scaling
    peak_score = jnp.maximum(lax.optimization_barrier(jnp.max(scores, axis=3)), self_score)
    cache_weight = jnp.exp(scores - peak_score[..., None])
    self_weight = jnp.exp(self_score - peak_score)
    denominator = lax.optimization_barrier(jnp.sum(cache_weight, axis=3)) + self_weight
    cache_probs = (cache_weight / denominator[..., None]).astype(jnp.bfloat16)
    self_probs = (self_weight / denominator).astype(jnp.bfloat16)
    attended = jnp.einsum('bgrl,blgd->bgrd', cache_probs.astype(jnp.float32), value_heads)
    attended = attended + self_probs.astype(jnp.float32)[..., None] * new_values.reshape(SEQUENCE_TOTAL, KEY_VALUE_HEADS, 1, HD).astype(jnp.float32)
    attended = attended.reshape(SEQUENCE_TOTAL, HEADS * HD).astype(jnp.bfloat16)
    residual = tokens.astype(jnp.float32) + jnp.dot(attended, w_attn_out, preferred_element_type=jnp.float32)
    second = norm_rows(residual, ffn_gain)
    branch_share = jax.nn.sigmoid(jnp.dot(second.astype(jnp.float32), branch_gate, precision=lax.Precision.HIGHEST))
    dense_hidden = swiglu(second, dense_gate, dense_up)
    dense = jnp.dot(dense_hidden, dense_down, preferred_element_type=jnp.float32)
    expert_ids = lax.broadcasted_iota(jnp.int32, (SEQUENCE_TOTAL, TOPK, EXPERTS), 2)
    weight_table = lax.optimization_barrier(jnp.sum(jnp.where(routes[:, :, None] == expert_ids, route_weights[:, :, None], 0.0), axis=1))
    limit = N_EP * CAP

    def one_expert(carried, index):
        own_column = lax.dynamic_index_in_dim(weight_table, index, 1, keepdims=False)
        picked = jnp.nonzero(own_column > 0.0, size=limit, fill_value=SEQUENCE_TOTAL)[0].astype(jnp.int32)
        clipped = jnp.minimum(picked, SEQUENCE_TOTAL - 1)
        answer = expert_rows(second[clipped], expert_gate[index], expert_up[index], expert_down[index])
        picked_weight = jnp.where(picked < SEQUENCE_TOTAL, own_column[clipped], 0.0)
        carried = carried.at[picked].add(picked_weight[:, None] * answer.astype(jnp.float32), mode='drop')
        return (carried, None)
    routed, _ = lax.scan(one_expert, jnp.zeros((SEQUENCE_TOTAL, D), jnp.float32), jnp.arange(EXPERTS, dtype=jnp.int32))
    return (residual + branch_share[:, None] * dense + routed).astype(jnp.bfloat16)
```

```python
import math

import jax
import jax.numpy as jnp
from jax import lax
from jax.experimental import pallas as pl
from jax.experimental.pallas import tpu as pltpu
from jax.sharding import PartitionSpec as P

EPSILON = 1e-06
LANES = 128
CORES = 2
SIDES = 2
CHUNKS = 4
MESH = pl.DeviceIdType.MESH


def exchange_kernel(
    count,
    depth,
    block_ref,
    residual_ref,
    branch_ref,
    dense_gate_hbm,
    dense_up_hbm,
    dense_down_hbm,
    expert_gate_hbm,
    expert_up_hbm,
    expert_down_hbm,
    out_ref,
    rows_buf,
    dense_gate,
    dense_up,
    dense_down,
    expert_gate,
    expert_up,
    expert_down,
    partial,
    core_out,
    core_in,
    side_out,
    side_in,
    depth_out,
    depth_in,
    kept,
    load_sem,
    gather_send,
    gather_recv,
    scatter_send,
    scatter_recv,
):
    me = lax.axis_index("ep")
    core = lax.rem(me, CORES)
    side = lax.rem(me // CORES, SIDES)
    level = me // (CORES * SIDES)
    own_rows, width = residual_ref.shape
    step = width // CHUNKS

    def device(level_at, side_at, core_at):
        return {"ep": level_at * (CORES * SIDES) + side_at * CORES + core_at}

    def away(distance):
        return lax.rem(level + distance, depth)

    def behind(distance):
        return lax.rem(level + depth - distance, depth)

    partner = device(level, side, 1 - core)
    across = device(level, 1 - side, core)

    loads = [
        pltpu.make_async_copy(source, target, load_sem.at[at])
        for at, (source, target) in enumerate(
            (
                (dense_gate_hbm, dense_gate),
                (dense_up_hbm, dense_up),
                (expert_gate_hbm.at[0], expert_gate),
                (expert_up_hbm.at[0], expert_up),
                (dense_down_hbm, dense_down),
                (expert_down_hbm.at[0], expert_down),
            )
        )
    ]
    for load in loads:
        load.start()

    barrier = pltpu.get_barrier_semaphore()
    for peer in [partner, across] + [device(away(d), side, core) for d in range(1, depth)]:
        pl.semaphore_signal(barrier, inc=1, device_id=peer, device_id_type=MESH)
    pl.semaphore_wait(barrier, depth + 1)

    started = []

    def send(source, target, send_sem, recv_sem, peer):
        copy = pltpu.make_async_remote_copy(
            src_ref=source,
            dst_ref=target,
            send_sem=send_sem,
            recv_sem=recv_sem,
            device_id=peer,
            device_id_type=MESH,
        )
        copy.start()
        started.append(copy)

    def arrive(target, recv_sem):
        pltpu.make_async_remote_copy(
            src_ref=target,
            dst_ref=target,
            send_sem=recv_sem,
            recv_sem=recv_sem,
            device_id=partner,
            device_id_type=MESH,
        ).wait_recv()

    side_at = depth - 1
    core_at = side_at + depth
    own_slot = rows_buf.at[core, side, level]

    def pass_on(source, slot, at, peer):
        send(source, slot, gather_send.at[at], gather_recv.at[at], peer)

    for d in range(1, depth):
        pass_on(block_ref, own_slot, d - 1, device(away(d), side, core))
    pass_on(block_ref, own_slot, side_at, across)
    pass_on(block_ref, own_slot, core_at, partner)
    rows_buf[core, side, level] = block_ref[...]
    for d in range(1, depth + 1):
        if d < depth:
            slot = rows_buf.at[core, side, behind(d)]
            arrive(slot, gather_recv.at[d - 1])
            pass_on(slot, slot, side_at + d, across)
            pass_on(slot, slot, core_at + d, partner)
        slot = rows_buf.at[core, 1 - side, behind(d - 1)]
        arrive(slot, gather_recv.at[side_at + d - 1])
        pass_on(slot, slot, core_at + depth + d - 1, partner)
    for d in range(depth):
        arrive(rows_buf.at[1 - core, side, behind(d)], gather_recv.at[core_at + d])
    for d in range(depth):
        arrive(rows_buf.at[1 - core, 1 - side, behind(d)], gather_recv.at[core_at + depth + d])

    gathered = rows_buf[...].reshape(count * own_rows, block_ref.shape[1])
    second = gathered[:, :width]
    extra = gathered[:, width:].astype(jnp.float32)
    lane = lax.broadcasted_iota(jnp.int32, extra.shape, 1)
    mine = (lane == me) | (lane == me + count) | (lane == me + 2 * count)
    weight = jnp.sum(jnp.where(mine, extra, 0.0), axis=1, keepdims=True)
    share = jax.nn.sigmoid(
        jnp.sum(second.astype(jnp.float32) * branch_ref[...], axis=1, keepdims=True)
    )

    def hidden(gate_ref, up_ref):
        gate_part = jnp.dot(second, gate_ref[...], preferred_element_type=jnp.float32)
        up_part = jnp.dot(second, up_ref[...], preferred_element_type=jnp.float32)
        return (jax.nn.silu(gate_part) * up_part).astype(jnp.bfloat16)

    loads[0].wait()
    loads[1].wait()
    dense_hidden = hidden(dense_gate, dense_up)
    loads[2].wait()
    loads[3].wait()
    expert_hidden = hidden(expert_gate, expert_up)
    loads[4].wait()
    loads[5].wait()

    def produce(j):
        columns = pl.ds(j * step, step)
        dense = jnp.dot(dense_hidden, dense_down[:, columns], preferred_element_type=jnp.float32)
        answer = jnp.dot(expert_hidden, expert_down[:, columns], preferred_element_type=jnp.float32)
        total = share * dense + weight * answer.astype(jnp.bfloat16).astype(jnp.float32)
        partial[j] = total.reshape(partial.shape[1:])
        core_out[j] = partial[j, 1 - core].astype(jnp.bfloat16)
        send(core_out.at[j], core_in.at[j], scatter_send.at[j, 0], scatter_recv.at[j, 0], partner)

    def to_side(j):
        arrive(core_in.at[j], scatter_recv.at[j, 0])
        other = partial[j, core, 1 - side] + core_in[j, 1 - side].astype(jnp.float32)
        side_out[j] = other.astype(jnp.bfloat16)
        send(side_out.at[j], side_in.at[j], scatter_send.at[j, 1], scatter_recv.at[j, 1], across)

    def to_depth(j):
        arrive(side_in.at[j], scatter_recv.at[j, 1])
        total = (
            partial[j, core, side]
            + core_in[j, side].astype(jnp.float32)
            + side_in[j].astype(jnp.float32)
        )
        kept[j] = total
        depth_out[j] = total.astype(jnp.bfloat16)
        for d in range(1, depth):
            send(
                depth_out.at[j, away(d)],
                depth_in.at[j, d - 1],
                scatter_send.at[j, 1 + d],
                scatter_recv.at[j, 1 + d],
                device(away(d), side, core),
            )

    def finish(j):
        columns = pl.ds(j * step, step)
        total = residual_ref[:, columns] + kept[j, level]
        for d in range(1, depth):
            arrive(depth_in.at[j, d - 1], scatter_recv.at[j, 1 + d])
            total = total + depth_in[j, d - 1].astype(jnp.float32)
        out_ref[:, columns] = total.astype(out_ref.dtype)

    for tick in range(CHUNKS + 3):
        for delay, stage in ((0, produce), (1, to_side), (2, to_depth), (3, finish)):
            if 0 <= tick - delay < CHUNKS:
                stage(tick - delay)
    for copy in started:
        copy.wait_send()


def exchange(block, residual, branch_gate, *weights):
    count = lax.axis_size("ep")
    depth = count // (CORES * SIDES)
    own_rows, width = residual.shape
    step = width // CHUNKS
    wide = block.shape[1]
    bf16 = jnp.bfloat16
    grid_rows = (depth, own_rows)
    gathers = depth - 1 + depth + SIDES * depth
    scatters = 1 + depth
    return pl.pallas_call(
        lambda *refs: exchange_kernel(count, depth, *refs),
        out_shape=jax.ShapeDtypeStruct((own_rows, width), bf16),
        in_specs=[pl.BlockSpec(memory_space=pltpu.VMEM)] * 3
        + [pl.BlockSpec(memory_space=pl.ANY)] * 6,
        out_specs=pl.BlockSpec(memory_space=pltpu.VMEM),
        scratch_shapes=[pltpu.VMEM((CORES, SIDES) + grid_rows + (wide,), bf16)]
        + [pltpu.VMEM(w.shape[-2:], bf16) for w in weights]
        + [
            pltpu.VMEM((CHUNKS, CORES, SIDES) + grid_rows + (step,), jnp.float32),
            pltpu.VMEM((CHUNKS, SIDES) + grid_rows + (step,), bf16),
            pltpu.VMEM((CHUNKS, SIDES) + grid_rows + (step,), bf16),
            pltpu.VMEM((CHUNKS,) + grid_rows + (step,), bf16),
            pltpu.VMEM((CHUNKS,) + grid_rows + (step,), bf16),
            pltpu.VMEM((CHUNKS,) + grid_rows + (step,), bf16),
            pltpu.VMEM((CHUNKS, depth - 1, own_rows, step), bf16),
            pltpu.VMEM((CHUNKS,) + grid_rows + (step,), jnp.float32),
            pltpu.SemaphoreType.DMA((6,)),
            pltpu.SemaphoreType.DMA((gathers,)),
            pltpu.SemaphoreType.DMA((gathers,)),
            pltpu.SemaphoreType.DMA((CHUNKS, scatters)),
            pltpu.SemaphoreType.DMA((CHUNKS, scatters)),
        ],
        compiler_params=pltpu.CompilerParams(
            collective_id=0, has_side_effects=True, vmem_limit_bytes=48 * 1024 * 1024
        ),
        name="exchange",
    )(block, residual, branch_gate.reshape(1, -1), *weights)


def norm_rows(inputs, gain_vec):
    widened = inputs.astype(jnp.float32)
    scaled = widened * lax.rsqrt(jnp.mean(widened * widened, axis=-1, keepdims=True) + EPSILON)
    return (scaled * gain_vec).astype(jnp.bfloat16)


def attend(
    normed,
    w_query,
    w_key,
    w_value,
    w_forget,
    forget_bias,
    cache_keys,
    cache_values,
    cache_logsum,
    lengths,
):
    own_rows = normed.shape[0]
    kv_heads = cache_logsum.shape[1]
    cache_span = cache_logsum.shape[2]
    head_size = w_key.shape[1] // kv_heads
    group_size = w_query.shape[1] // head_size // kv_heads
    scaling = 1.0 / math.sqrt(head_size)
    queries = jnp.dot(normed, w_query, preferred_element_type=jnp.float32).astype(jnp.bfloat16)
    new_keys = jnp.dot(normed, w_key, preferred_element_type=jnp.float32).astype(jnp.bfloat16)
    new_values = jnp.dot(normed, w_value, preferred_element_type=jnp.float32).astype(jnp.bfloat16)
    log_gate = jax.nn.log_sigmoid(
        jnp.dot(normed, w_forget, preferred_element_type=jnp.float32) + forget_bias
    )
    positions = lax.broadcasted_iota(jnp.int32, (own_rows, kv_heads, cache_span), 2)
    latest = jnp.sum(jnp.where(positions == lengths[:, None, None] - 1, cache_logsum, 0.0), axis=2)
    offsets = (latest + log_gate)[:, :, None] - cache_logsum
    usable = positions < lengths[:, None, None]
    query_heads = queries.reshape(own_rows, kv_heads, group_size, head_size)
    key_heads = cache_keys.reshape(own_rows, cache_span, kv_heads, head_size)
    value_heads = cache_values.reshape(own_rows, cache_span, kv_heads, head_size)
    scores = (
        jnp.einsum("bgrd,blgd->bgrl", query_heads, key_heads, preferred_element_type=jnp.float32)
        * scaling
    )
    scores = jnp.where(usable[:, :, None, :], scores + offsets[:, :, None, :], -jnp.inf)
    self_score = (
        jnp.einsum(
            "bgrd,bgd->bgr",
            query_heads,
            new_keys.reshape(own_rows, kv_heads, head_size),
            preferred_element_type=jnp.float32,
        )
        * scaling
    )
    peak_score = jnp.maximum(jnp.max(scores, axis=3), self_score)
    cache_weight = jnp.exp(scores - peak_score[..., None])
    self_weight = jnp.exp(self_score - peak_score)
    denominator = jnp.sum(cache_weight, axis=3) + self_weight
    cache_probs = (cache_weight / denominator[..., None]).astype(jnp.bfloat16)
    self_probs = (self_weight / denominator).astype(jnp.bfloat16)
    attended = jnp.einsum(
        "bgrl,blgd->bgrd", cache_probs, value_heads, preferred_element_type=jnp.float32
    )
    attended = attended + self_probs.astype(jnp.float32)[..., None] * new_values.reshape(
        own_rows, kv_heads, 1, head_size
    ).astype(jnp.float32)
    return attended.reshape(own_rows, -1).astype(jnp.bfloat16)


def body(
    tokens,
    attn_gain,
    w_query,
    w_key,
    w_value,
    w_forget,
    forget_bias,
    w_attn_out,
    cache_keys,
    cache_values,
    cache_logsum,
    lengths,
    ffn_gain,
    branch_gate,
    dense_gate,
    dense_up,
    dense_down,
    expert_gate,
    expert_up,
    expert_down,
    routes,
    route_weights,
):
    own_rows = tokens.shape[0]
    normed = norm_rows(tokens, attn_gain)
    attended = attend(
        normed,
        w_query,
        w_key,
        w_value,
        w_forget,
        forget_bias,
        cache_keys,
        cache_values,
        cache_logsum,
        lengths,
    )
    residual = tokens.astype(jnp.float32) + jnp.dot(
        attended, w_attn_out, preferred_element_type=jnp.float32
    )
    second = norm_rows(residual, ffn_gain)
    count = lax.axis_size("ep")
    routed_to = routes[:, :, None] == lax.broadcasted_iota(jnp.int32, routes.shape + (count,), 2)
    table = jnp.sum(jnp.where(routed_to, route_weights[:, :, None], 0.0), axis=1)
    high = lax.reduce_precision(table, 8, 7)
    middle = lax.reduce_precision(table - high, 8, 7)
    extra = jnp.concatenate([high, middle, table - high - middle], axis=1)
    extra = jnp.pad(extra, ((0, 0), (0, -extra.shape[1] % LANES))).astype(jnp.bfloat16)
    return exchange(
        jnp.concatenate([second, extra], axis=1),
        residual,
        branch_gate,
        dense_gate,
        dense_up,
        dense_down,
        expert_gate,
        expert_up,
        expert_down,
    )


def solution(mesh):
    return jax.shard_map(
        body,
        mesh=mesh,
        in_specs=(
            P(("grp", "ep"), None),
            P(),
            P(),
            P(),
            P(),
            P(),
            P(),
            P(),
            P(("grp", "ep"), None, None),
            P(("grp", "ep"), None, None),
            P(("grp", "ep"), None, None),
            P(("grp", "ep")),
            P(),
            P(),
            P(None, "ep"),
            P(None, "ep"),
            P("ep", None),
            P("ep", None, None),
            P("ep", None, None),
            P("ep", None, None),
            P(("grp", "ep"), None),
            P(("grp", "ep"), None),
        ),
        out_specs=P(("grp", "ep"), None),
        check_vma=False,
    )
```

```python
import math

import jax
import jax.numpy as jnp
from jax import lax
from jax.experimental import pallas as pl
from jax.experimental.pallas import tpu as pltpu
from jax.sharding import PartitionSpec as P

EPSILON = 1e-06
LANES = 128
CORES = 2
SIDES = 2
CHUNKS = 4
GROUP = 4
MESH = pl.DeviceIdType.MESH


def exchange_kernel(
    count,
    depth,
    block_ref,
    residual_ref,
    branch_ref,
    dense_gate_hbm,
    dense_up_hbm,
    dense_down_hbm,
    expert_gate_hbm,
    expert_up_hbm,
    expert_down_hbm,
    out_ref,
    rows_buf,
    dense_gate,
    dense_up,
    dense_down,
    expert_gate,
    expert_up,
    expert_down,
    partial,
    core_out,
    core_in,
    side_out,
    side_in,
    depth_out,
    depth_in,
    kept,
    load_sem,
    gather_send,
    gather_recv,
    scatter_send,
    scatter_recv,
):
    me = lax.axis_index("ep")
    core = lax.rem(me, CORES)
    side = lax.rem(me // CORES, SIDES)
    level = me // (CORES * SIDES)
    own_rows, width = residual_ref.shape
    step = width // CHUNKS

    def device(level_at, side_at, core_at):
        return {"ep": level_at * (CORES * SIDES) + side_at * CORES + core_at}

    def away(distance):
        return lax.rem(level + distance, depth)

    def behind(distance):
        return lax.rem(level + depth - distance, depth)

    partner = device(level, side, 1 - core)
    across = device(level, 1 - side, core)

    loads = [
        pltpu.make_async_copy(source, target, load_sem.at[at])
        for at, (source, target) in enumerate(
            (
                (dense_gate_hbm, dense_gate),
                (dense_up_hbm, dense_up),
                (expert_gate_hbm.at[0], expert_gate),
                (expert_up_hbm.at[0], expert_up),
                (dense_down_hbm, dense_down),
                (expert_down_hbm.at[0], expert_down),
            )
        )
    ]
    for load in loads:
        load.start()

    barrier = pltpu.get_barrier_semaphore()
    for peer in [partner, across] + [device(away(d), side, core) for d in range(1, depth)]:
        pl.semaphore_signal(barrier, inc=1, device_id=peer, device_id_type=MESH)
    pl.semaphore_wait(barrier, depth + 1)

    started = []

    def send(source, target, send_sem, recv_sem, peer):
        copy = pltpu.make_async_remote_copy(
            src_ref=source,
            dst_ref=target,
            send_sem=send_sem,
            recv_sem=recv_sem,
            device_id=peer,
            device_id_type=MESH,
        )
        copy.start()
        started.append(copy)

    def arrive(target, recv_sem):
        pltpu.make_async_remote_copy(
            src_ref=target,
            dst_ref=target,
            send_sem=recv_sem,
            recv_sem=recv_sem,
            device_id=partner,
            device_id_type=MESH,
        ).wait_recv()

    side_at = depth - 1
    core_at = side_at + depth
    own_slot = rows_buf.at[core, side, level]

    def pass_on(source, slot, at, peer):
        send(source, slot, gather_send.at[at], gather_recv.at[at], peer)

    for d in range(1, depth):
        pass_on(block_ref, own_slot, d - 1, device(away(d), side, core))
    pass_on(block_ref, own_slot, side_at, across)
    pass_on(block_ref, own_slot, core_at, partner)
    rows_buf[core, side, level] = block_ref[...]
    for d in range(1, depth + 1):
        if d < depth:
            slot = rows_buf.at[core, side, behind(d)]
            arrive(slot, gather_recv.at[d - 1])
            pass_on(slot, slot, side_at + d, across)
            pass_on(slot, slot, core_at + d, partner)
        slot = rows_buf.at[core, 1 - side, behind(d - 1)]
        arrive(slot, gather_recv.at[side_at + d - 1])
        pass_on(slot, slot, core_at + depth + d - 1, partner)
    for d in range(depth):
        arrive(rows_buf.at[1 - core, side, behind(d)], gather_recv.at[core_at + d])
    for d in range(depth):
        arrive(rows_buf.at[1 - core, 1 - side, behind(d)], gather_recv.at[core_at + depth + d])

    gathered = rows_buf[...].reshape(count * own_rows, block_ref.shape[1])
    second = gathered[:, :width]
    extra = gathered[:, width:].astype(jnp.float32)
    lane = lax.broadcasted_iota(jnp.int32, extra.shape, 1)
    mine = (lane == me) | (lane == me + count) | (lane == me + 2 * count)
    weight = jnp.sum(jnp.where(mine, extra, 0.0), axis=1, keepdims=True)
    share = jax.nn.sigmoid(
        jnp.sum(second.astype(jnp.float32) * branch_ref[...], axis=1, keepdims=True)
    )

    def hidden(gate_ref, up_ref):
        gate_part = jnp.dot(second, gate_ref[...], preferred_element_type=jnp.float32)
        up_part = jnp.dot(second, up_ref[...], preferred_element_type=jnp.float32)
        return (jax.nn.silu(gate_part) * up_part).astype(jnp.bfloat16)

    loads[0].wait()
    loads[1].wait()
    dense_hidden = hidden(dense_gate, dense_up)
    loads[2].wait()
    loads[3].wait()
    expert_hidden = hidden(expert_gate, expert_up)
    loads[4].wait()
    loads[5].wait()

    def produce(j):
        columns = pl.ds(j * step, step)
        dense = jnp.dot(dense_hidden, dense_down[:, columns], preferred_element_type=jnp.float32)
        answer = jnp.dot(expert_hidden, expert_down[:, columns], preferred_element_type=jnp.float32)
        total = share * dense + weight * answer.astype(jnp.bfloat16).astype(jnp.float32)
        partial[j] = total.reshape(partial.shape[1:])
        core_out[j] = partial[j, 1 - core].astype(jnp.bfloat16)
        send(core_out.at[j], core_in.at[j], scatter_send.at[j, 0], scatter_recv.at[j, 0], partner)

    def to_side(j):
        arrive(core_in.at[j], scatter_recv.at[j, 0])
        other = partial[j, core, 1 - side] + core_in[j, 1 - side].astype(jnp.float32)
        side_out[j] = other.astype(jnp.bfloat16)
        send(side_out.at[j], side_in.at[j], scatter_send.at[j, 1], scatter_recv.at[j, 1], across)

    def to_depth(j):
        arrive(side_in.at[j], scatter_recv.at[j, 1])
        total = (
            partial[j, core, side]
            + core_in[j, side].astype(jnp.float32)
            + side_in[j].astype(jnp.float32)
        )
        kept[j] = total
        depth_out[j] = total.astype(jnp.bfloat16)
        for d in range(1, depth):
            send(
                depth_out.at[j, away(d)],
                depth_in.at[j, d - 1],
                scatter_send.at[j, 1 + d],
                scatter_recv.at[j, 1 + d],
                device(away(d), side, core),
            )

    def finish(j):
        columns = pl.ds(j * step, step)
        total = residual_ref[:, columns] + kept[j, level]
        for d in range(1, depth):
            arrive(depth_in.at[j, d - 1], scatter_recv.at[j, 1 + d])
            total = total + depth_in[j, d - 1].astype(jnp.float32)
        out_ref[:, columns] = total.astype(out_ref.dtype)

    for tick in range(CHUNKS + 3):
        for delay, stage in ((0, produce), (1, to_side), (2, to_depth), (3, finish)):
            if 0 <= tick - delay < CHUNKS:
                stage(tick - delay)
    for copy in started:
        copy.wait_send()


def exchange(block, residual, branch_gate, *weights):
    count = lax.axis_size("ep")
    depth = count // (CORES * SIDES)
    own_rows, width = residual.shape
    step = width // CHUNKS
    wide = block.shape[1]
    bf16 = jnp.bfloat16
    grid_rows = (depth, own_rows)
    gathers = depth - 1 + depth + SIDES * depth
    scatters = 1 + depth
    return pl.pallas_call(
        lambda *refs: exchange_kernel(count, depth, *refs),
        out_shape=jax.ShapeDtypeStruct((own_rows, width), bf16),
        in_specs=[pl.BlockSpec(memory_space=pltpu.VMEM)] * 3
        + [pl.BlockSpec(memory_space=pl.ANY)] * 6,
        out_specs=pl.BlockSpec(memory_space=pltpu.VMEM),
        scratch_shapes=[pltpu.VMEM((CORES, SIDES) + grid_rows + (wide,), bf16)]
        + [pltpu.VMEM(w.shape[-2:], bf16) for w in weights]
        + [
            pltpu.VMEM((CHUNKS, CORES, SIDES) + grid_rows + (step,), jnp.float32),
            pltpu.VMEM((CHUNKS, SIDES) + grid_rows + (step,), bf16),
            pltpu.VMEM((CHUNKS, SIDES) + grid_rows + (step,), bf16),
            pltpu.VMEM((CHUNKS,) + grid_rows + (step,), bf16),
            pltpu.VMEM((CHUNKS,) + grid_rows + (step,), bf16),
            pltpu.VMEM((CHUNKS,) + grid_rows + (step,), bf16),
            pltpu.VMEM((CHUNKS, depth - 1, own_rows, step), bf16),
            pltpu.VMEM((CHUNKS,) + grid_rows + (step,), jnp.float32),
            pltpu.SemaphoreType.DMA((6,)),
            pltpu.SemaphoreType.DMA((gathers,)),
            pltpu.SemaphoreType.DMA((gathers,)),
            pltpu.SemaphoreType.DMA((CHUNKS, scatters)),
            pltpu.SemaphoreType.DMA((CHUNKS, scatters)),
        ],
        compiler_params=pltpu.CompilerParams(
            collective_id=0, has_side_effects=True, vmem_limit_bytes=48 * 1024 * 1024
        ),
        name="exchange",
    )(block, residual, branch_gate.reshape(1, -1), *weights)


def attend_kernel(
    count,
    tokens_ref,
    attn_gain_ref,
    w_query_hbm,
    w_key_hbm,
    w_value_hbm,
    w_forget_ref,
    forget_bias_ref,
    w_attn_out_hbm,
    keys_hbm,
    values_hbm,
    logsum_ref,
    lengths_ref,
    ffn_gain_ref,
    routes_ref,
    route_weights_ref,
    residual_ref,
    block_ref,
    w_query,
    w_key,
    w_value,
    w_attn_out,
    keys,
    values,
    query_rows,
    new_keys,
    new_values,
    gates,
    attended_rows,
    weight_sem,
    cache_sem,
):
    own_rows, width = tokens_ref.shape
    kv_heads, span = logsum_ref.shape[1:]
    head_size = w_key.shape[1] // kv_heads
    scaling = 1.0 / math.sqrt(head_size)
    pieces = query_rows.shape[1]

    loads = [
        pltpu.make_async_copy(source, target, weight_sem.at[at])
        for at, (source, target) in enumerate(
            (
                (w_query_hbm, w_query),
                (w_key_hbm, w_key),
                (w_value_hbm, w_value),
                (w_attn_out_hbm, w_attn_out),
            )
        )
    ]

    def cache_loads(at):
        members = pl.ds(at * GROUP, GROUP)
        return (
            pltpu.make_async_copy(keys_hbm.at[members], keys.at[members], cache_sem.at[at, 0]),
            pltpu.make_async_copy(values_hbm.at[members], values.at[members], cache_sem.at[at, 1]),
        )

    for load in loads[:3]:
        load.start()
    for at in range(own_rows // GROUP):
        for load in cache_loads(at):
            load.start()
    loads[3].start()

    def normalise(widened, gain):
        mean = jnp.mean(widened * widened, axis=-1, keepdims=True)
        return (widened * lax.rsqrt(mean + EPSILON) * gain).astype(jnp.bfloat16)

    tokens = tokens_ref[...].astype(jnp.float32)
    normed = normalise(tokens, attn_gain_ref[...])
    wide_normed = normed.astype(jnp.float32)
    for head in range(kv_heads):
        row = w_forget_ref[pl.ds(head, 1), :].astype(jnp.float32)
        logit = jnp.sum(wide_normed * row, axis=1, keepdims=True) + forget_bias_ref[head]
        log_gate = jnp.minimum(logit, 0.0) - jnp.log1p(jnp.exp(-jnp.abs(logit)))
        gates[:, head, :] = jnp.broadcast_to(log_gate, (own_rows, gates.shape[2]))

    def project(weights):
        product = jnp.dot(normed, weights[...], preferred_element_type=jnp.float32)
        return product.astype(jnp.bfloat16).astype(jnp.float32)

    loads[0].wait()
    queries = project(w_query)
    for piece in range(pieces):
        query_rows[:, piece, :] = queries[:, piece * LANES : (piece + 1) * LANES]
    loads[1].wait()
    new_keys[...] = project(w_key)
    loads[2].wait()
    new_values[...] = project(w_value)

    piece_at = lax.broadcasted_iota(jnp.int32, (pieces, LANES), 0)
    lane_at = lax.broadcasted_iota(jnp.int32, (pieces, LANES), 1)
    in_place = (piece_at < pieces // kv_heads) == (lane_at < head_size)
    row_at = lax.rem(lax.broadcasted_iota(jnp.int32, (2 * pieces, span), 0), pieces)
    early = row_at < pieces // kv_heads
    position = lax.broadcasted_iota(jnp.int32, (2 * pieces, span), 1)
    head_position = lax.broadcasted_iota(jnp.int32, (kv_heads, span), 1)

    def sequence(b):
        valid = lengths_ref[b]
        plain = query_rows[b]
        turned = pltpu.roll(plain, head_size, 1)
        query = jnp.concatenate(
            [jnp.where(in_place, plain, 0.0), jnp.where(in_place, turned, 0.0)], axis=0
        )
        scores = lax.dot_general(
            query.astype(jnp.bfloat16),
            keys[b],
            (((1,), (1,)), ((), ())),
            preferred_element_type=jnp.float32,
        )
        logsum = logsum_ref[b]
        latest = jnp.sum(jnp.where(head_position == valid - 1, logsum, 0.0), axis=1, keepdims=True)
        offsets = (latest + gates[b][:, :1]) - logsum
        offset = jnp.where(early, offsets[0:1, :], offsets[1:2, :])
        scores = jnp.where(position < valid, scores * scaling + offset, -jnp.inf)
        own = jnp.sum(query * new_keys[pl.ds(b, 1), :], axis=1, keepdims=True) * scaling
        peak = jnp.maximum(jnp.max(scores, axis=1, keepdims=True), own)
        weight = jnp.exp(scores - peak)
        own_weight = jnp.exp(own - peak)
        inverse = 1.0 / (jnp.sum(weight, axis=1, keepdims=True) + own_weight)
        probs = (weight * inverse).astype(jnp.bfloat16)
        own_prob = (own_weight * inverse).astype(jnp.bfloat16).astype(jnp.float32)
        mixed = jnp.dot(probs, values[b], preferred_element_type=jnp.float32)
        mixed = mixed + own_prob * new_values[pl.ds(b, 1), :]
        first = jnp.where(in_place, mixed[:pieces], 0.0)
        other = jnp.where(in_place, mixed[pieces:], 0.0)
        return first + pltpu.roll(other, head_size, 1)

    def group(at, carried):
        for load in cache_loads(at):
            load.wait()
        results = [sequence(at * GROUP + member) for member in range(GROUP)]
        for member in range(GROUP):
            attended_rows[at * GROUP + member] = results[member]
        return carried

    lax.fori_loop(0, own_rows // GROUP, group, 0)

    attended = jnp.concatenate([attended_rows[:, piece, :] for piece in range(pieces)], axis=1)
    loads[3].wait()
    residual = tokens + jnp.dot(
        attended.astype(jnp.bfloat16), w_attn_out[...], preferred_element_type=jnp.float32
    )
    residual_ref[...] = residual
    block_ref[:, :width] = normalise(residual, ffn_gain_ref[...])
    lane = lax.broadcasted_iota(jnp.int32, (own_rows, block_ref.shape[1] - width), 1)
    table = jnp.zeros(lane.shape, jnp.float32)
    for k in range(routes_ref.shape[1]):
        chosen = lax.rem(lane, count) == routes_ref[:, k : k + 1]
        table = table + jnp.where(chosen, route_weights_ref[:, k : k + 1], 0.0)
    high = table.astype(jnp.bfloat16).astype(jnp.float32)
    middle = (table - high).astype(jnp.bfloat16).astype(jnp.float32)
    extra = jnp.where(lane < count, high, jnp.where(lane < 2 * count, middle, table - high - middle))
    block_ref[:, width:] = extra.astype(jnp.bfloat16)


def attend(
    tokens,
    attn_gain,
    w_query,
    w_key,
    w_value,
    w_forget,
    forget_bias,
    w_attn_out,
    cache_keys,
    cache_values,
    cache_logsum,
    lengths,
    ffn_gain,
    routes,
    route_weights,
):
    count = lax.axis_size("ep")
    own_rows, width = tokens.shape
    kv_heads = cache_logsum.shape[1]
    pieces = w_query.shape[1] // LANES
    wide = width + -(-3 * count // LANES) * LANES
    bf16, f32 = jnp.bfloat16, jnp.float32
    near = pl.BlockSpec(memory_space=pltpu.VMEM)
    far = pl.BlockSpec(memory_space=pl.ANY)
    scalars = pl.BlockSpec(memory_space=pltpu.SMEM)
    return pl.pallas_call(
        lambda *refs: attend_kernel(count, *refs),
        out_shape=(
            jax.ShapeDtypeStruct((own_rows, width), f32),
            jax.ShapeDtypeStruct((own_rows, wide), bf16),
        ),
        in_specs=[near, near, far, far, far, near, scalars, far, far, far, near, scalars]
        + [near, near, near],
        out_specs=(near, near),
        scratch_shapes=[
            pltpu.VMEM(w_query.shape, bf16),
            pltpu.VMEM(w_key.shape, bf16),
            pltpu.VMEM(w_value.shape, bf16),
            pltpu.VMEM(w_attn_out.shape, bf16),
            pltpu.VMEM(cache_keys.shape, bf16),
            pltpu.VMEM(cache_values.shape, bf16),
            pltpu.VMEM((own_rows, pieces, LANES), f32),
            pltpu.VMEM((own_rows, w_key.shape[1]), f32),
            pltpu.VMEM((own_rows, w_value.shape[1]), f32),
            pltpu.VMEM((own_rows, kv_heads, LANES), f32),
            pltpu.VMEM((own_rows, pieces, LANES), f32),
            pltpu.SemaphoreType.DMA((4,)),
            pltpu.SemaphoreType.DMA((own_rows // GROUP, 2)),
        ],
        compiler_params=pltpu.CompilerParams(vmem_limit_bytes=40 * 1024 * 1024),
        name="attend",
    )(
        tokens,
        attn_gain.reshape(1, -1),
        w_query,
        w_key,
        w_value,
        w_forget.T,
        forget_bias,
        w_attn_out,
        cache_keys,
        cache_values,
        cache_logsum,
        lengths,
        ffn_gain.reshape(1, -1),
        routes,
        route_weights,
    )


def body(
    tokens,
    attn_gain,
    w_query,
    w_key,
    w_value,
    w_forget,
    forget_bias,
    w_attn_out,
    cache_keys,
    cache_values,
    cache_logsum,
    lengths,
    ffn_gain,
    branch_gate,
    dense_gate,
    dense_up,
    dense_down,
    expert_gate,
    expert_up,
    expert_down,
    routes,
    route_weights,
):
    residual, block = attend(
        tokens,
        attn_gain,
        w_query,
        w_key,
        w_value,
        w_forget,
        forget_bias,
        w_attn_out,
        cache_keys,
        cache_values,
        cache_logsum,
        lengths,
        ffn_gain,
        routes,
        route_weights,
    )
    return exchange(
        block,
        residual,
        branch_gate,
        dense_gate,
        dense_up,
        dense_down,
        expert_gate,
        expert_up,
        expert_down,
    )


def solution(mesh):
    return jax.shard_map(
        body,
        mesh=mesh,
        in_specs=(
            P(("grp", "ep"), None),
            P(),
            P(),
            P(),
            P(),
            P(),
            P(),
            P(),
            P(("grp", "ep"), None, None),
            P(("grp", "ep"), None, None),
            P(("grp", "ep"), None, None),
            P(("grp", "ep")),
            P(),
            P(),
            P(None, "ep"),
            P(None, "ep"),
            P("ep", None),
            P("ep", None, None),
            P("ep", None, None),
            P("ep", None, None),
            P(("grp", "ep"), None),
            P(("grp", "ep"), None),
        ),
        out_specs=P(("grp", "ep"), None),
        check_vma=False,
    )
```

```python
import math

import jax
import jax.numpy as jnp
from jax import lax
from jax.experimental import pallas as pl
from jax.experimental.pallas import tpu as pltpu
from jax.sharding import PartitionSpec as P

EPSILON = 1e-06
LANES = 128
CORES = 2
SIDES = 2
CHUNKS = 2
GROUP = 8
VMEM_BYTES = 67043328
MESH = pl.DeviceIdType.MESH


def exchange_kernel(
    count,
    depth,
    block_ref,
    residual_ref,
    branch_ref,
    dense_gate_hbm,
    dense_up_hbm,
    dense_down_hbm,
    expert_gate_hbm,
    expert_up_hbm,
    expert_down_hbm,
    out_ref,
    rows_buf,
    dense_gate,
    dense_up,
    dense_down,
    expert_gate,
    expert_up,
    expert_down,
    partial,
    core_out,
    core_in,
    side_out,
    side_in,
    depth_out,
    depth_in,
    kept,
    load_sem,
    gather_send,
    gather_recv,
    scatter_send,
    scatter_recv,
):
    me = lax.axis_index("ep")
    core = lax.rem(me, CORES)
    side = lax.rem(me // CORES, SIDES)
    level = me // (CORES * SIDES)
    own_rows, width = residual_ref.shape
    step = width // CHUNKS

    def device(level_at, side_at, core_at):
        return {"ep": level_at * (CORES * SIDES) + side_at * CORES + core_at}

    def away(distance):
        return lax.rem(level + distance, depth)

    def behind(distance):
        return lax.rem(level + depth - distance, depth)

    partner = device(level, side, 1 - core)
    across = device(level, 1 - side, core)

    loads = [
        pltpu.make_async_copy(source, target, load_sem.at[at])
        for at, (source, target) in enumerate(
            (
                (dense_gate_hbm, dense_gate),
                (dense_up_hbm, dense_up),
                (expert_gate_hbm.at[0], expert_gate),
                (expert_up_hbm.at[0], expert_up),
                (dense_down_hbm, dense_down),
                (expert_down_hbm.at[0], expert_down),
            )
        )
    ]
    for load in loads:
        load.start()

    barrier = pltpu.get_barrier_semaphore()
    for peer in [partner, across] + [device(away(d), side, core) for d in range(1, depth)]:
        pl.semaphore_signal(barrier, inc=1, device_id=peer, device_id_type=MESH)
    pl.semaphore_wait(barrier, depth + 1)

    started = []

    def send(source, target, send_sem, recv_sem, peer):
        copy = pltpu.make_async_remote_copy(
            src_ref=source,
            dst_ref=target,
            send_sem=send_sem,
            recv_sem=recv_sem,
            device_id=peer,
            device_id_type=MESH,
        )
        copy.start()
        started.append(copy)

    def arrive(target, recv_sem):
        pltpu.make_async_remote_copy(
            src_ref=target,
            dst_ref=target,
            send_sem=recv_sem,
            recv_sem=recv_sem,
            device_id=partner,
            device_id_type=MESH,
        ).wait_recv()

    side_at = depth - 1
    core_at = side_at + depth
    own_slot = rows_buf.at[core, side, level]

    def pass_on(source, slot, at, peer):
        send(source, slot, gather_send.at[at], gather_recv.at[at], peer)

    pass_on(block_ref, own_slot, side_at, across)
    pass_on(block_ref, own_slot, core_at, partner)
    for d in range(1, depth):
        pass_on(block_ref, own_slot, d - 1, device(away(d), side, core))
    rows_buf[core, side, level] = block_ref[...]
    for d in range(1, depth + 1):
        if d < depth:
            slot = rows_buf.at[core, side, behind(d)]
            arrive(slot, gather_recv.at[d - 1])
            pass_on(slot, slot, side_at + d, across)
            pass_on(slot, slot, core_at + d, partner)
        slot = rows_buf.at[core, 1 - side, behind(d - 1)]
        arrive(slot, gather_recv.at[side_at + d - 1])
        pass_on(slot, slot, core_at + depth + d - 1, partner)
    for load in loads[:4]:
        load.wait()

    def hidden(group, gate_ref, up_ref):
        rows = rows_buf[group].reshape(count // CORES * own_rows, block_ref.shape[1])[:, :width]
        gate_part = jnp.dot(rows, gate_ref[...], preferred_element_type=jnp.float32)
        up_part = jnp.dot(rows, up_ref[...], preferred_element_type=jnp.float32)
        return jax.nn.silu(gate_part) * up_part

    def in_order(near, distant):
        ahead = jnp.where(core == 0, near, distant)
        after = jnp.where(core == 0, distant, near)
        return jnp.concatenate([ahead, after], axis=0).astype(jnp.bfloat16)

    near_dense = hidden(core, dense_gate, dense_up)
    near_expert = hidden(core, expert_gate, expert_up)
    for d in range(depth):
        arrive(rows_buf.at[1 - core, side, behind(d)], gather_recv.at[core_at + d])
    for d in range(depth):
        arrive(rows_buf.at[1 - core, 1 - side, behind(d)], gather_recv.at[core_at + depth + d])

    gathered = rows_buf[...].reshape(count * own_rows, block_ref.shape[1])
    second = gathered[:, :width]
    extra = gathered[:, width:].astype(jnp.float32)
    lane = lax.broadcasted_iota(jnp.int32, extra.shape, 1)
    mine = (lane == me) | (lane == me + count) | (lane == me + 2 * count)
    weight = jnp.sum(jnp.where(mine, extra, 0.0), axis=1, keepdims=True)
    share = jax.nn.sigmoid(
        jnp.sum(second.astype(jnp.float32) * branch_ref[...], axis=1, keepdims=True)
    )

    dense_hidden = in_order(near_dense, hidden(1 - core, dense_gate, dense_up))
    expert_hidden = in_order(near_expert, hidden(1 - core, expert_gate, expert_up))
    loads[4].wait()
    loads[5].wait()

    def produce(j):
        columns = pl.ds(j * step, step)
        dense = jnp.dot(dense_hidden, dense_down[:, columns], preferred_element_type=jnp.float32)
        answer = jnp.dot(expert_hidden, expert_down[:, columns], preferred_element_type=jnp.float32)
        total = share * dense + weight * answer.astype(jnp.bfloat16).astype(jnp.float32)
        partial[j] = total.reshape(partial.shape[1:])
        core_out[j] = partial[j, 1 - core].astype(jnp.bfloat16)
        send(core_out.at[j], core_in.at[j], scatter_send.at[j, 0], scatter_recv.at[j, 0], partner)

    def to_side(j):
        arrive(core_in.at[j], scatter_recv.at[j, 0])
        other = partial[j, core, 1 - side] + core_in[j, 1 - side].astype(jnp.float32)
        side_out[j] = other.astype(jnp.bfloat16)
        send(side_out.at[j], side_in.at[j], scatter_send.at[j, 1], scatter_recv.at[j, 1], across)

    def to_depth(j):
        arrive(side_in.at[j], scatter_recv.at[j, 1])
        total = (
            partial[j, core, side]
            + core_in[j, side].astype(jnp.float32)
            + side_in[j].astype(jnp.float32)
        )
        kept[j] = total
        depth_out[j] = total.astype(jnp.bfloat16)
        for d in range(1, depth):
            send(
                depth_out.at[j, away(d)],
                depth_in.at[j, d - 1],
                scatter_send.at[j, 1 + d],
                scatter_recv.at[j, 1 + d],
                device(away(d), side, core),
            )

    def finish(j):
        columns = pl.ds(j * step, step)
        total = residual_ref[:, columns] + kept[j, level]
        for d in range(1, depth):
            arrive(depth_in.at[j, d - 1], scatter_recv.at[j, 1 + d])
            total = total + depth_in[j, d - 1].astype(jnp.float32)
        out_ref[:, columns] = total.astype(out_ref.dtype)

    for tick in range(CHUNKS + 3):
        for delay, stage in ((0, produce), (1, to_side), (2, to_depth), (3, finish)):
            if 0 <= tick - delay < CHUNKS:
                stage(tick - delay)
    for copy in started:
        copy.wait_send()


def exchange(block, residual, branch_gate, *weights):
    count = lax.axis_size("ep")
    depth = count // (CORES * SIDES)
    own_rows, width = residual.shape
    step = width // CHUNKS
    wide = block.shape[1]
    bf16 = jnp.bfloat16
    grid_rows = (depth, own_rows)
    gathers = depth - 1 + depth + SIDES * depth
    scatters = 1 + depth
    return pl.pallas_call(
        lambda *refs: exchange_kernel(count, depth, *refs),
        out_shape=jax.ShapeDtypeStruct((own_rows, width), bf16),
        in_specs=[pl.BlockSpec(memory_space=pltpu.VMEM)] * 3
        + [pl.BlockSpec(memory_space=pl.ANY)] * 6,
        out_specs=pl.BlockSpec(memory_space=pltpu.VMEM),
        scratch_shapes=[pltpu.VMEM((CORES, SIDES) + grid_rows + (wide,), bf16)]
        + [pltpu.VMEM(w.shape[-2:], bf16) for w in weights]
        + [
            pltpu.VMEM((CHUNKS, CORES, SIDES) + grid_rows + (step,), jnp.float32),
            pltpu.VMEM((CHUNKS, SIDES) + grid_rows + (step,), bf16),
            pltpu.VMEM((CHUNKS, SIDES) + grid_rows + (step,), bf16),
            pltpu.VMEM((CHUNKS,) + grid_rows + (step,), bf16),
            pltpu.VMEM((CHUNKS,) + grid_rows + (step,), bf16),
            pltpu.VMEM((CHUNKS,) + grid_rows + (step,), bf16),
            pltpu.VMEM((CHUNKS, depth - 1, own_rows, step), bf16),
            pltpu.VMEM((CHUNKS,) + grid_rows + (step,), jnp.float32),
            pltpu.SemaphoreType.DMA((6,)),
            pltpu.SemaphoreType.DMA((gathers,)),
            pltpu.SemaphoreType.DMA((gathers,)),
            pltpu.SemaphoreType.DMA((CHUNKS, scatters)),
            pltpu.SemaphoreType.DMA((CHUNKS, scatters)),
        ],
        compiler_params=pltpu.CompilerParams(
            collective_id=0, has_side_effects=True, vmem_limit_bytes=VMEM_BYTES
        ),
        name="exchange",
    )(block, residual, branch_gate.reshape(1, -1), *weights)


def attend_kernel(
    count,
    tokens_ref,
    attn_gain_ref,
    w_query_hbm,
    w_key_hbm,
    w_value_hbm,
    w_forget_ref,
    forget_bias_ref,
    w_attn_out_hbm,
    keys_hbm,
    values_hbm,
    logsum_ref,
    lengths_ref,
    ffn_gain_ref,
    routes_ref,
    route_weights_ref,
    residual_ref,
    block_ref,
    w_query,
    w_key,
    w_value,
    w_attn_out,
    keys,
    values,
    query_rows,
    new_keys,
    new_values,
    gates,
    attended_rows,
    extra_rows,
    weight_sem,
    cache_sem,
):
    own_rows, width = tokens_ref.shape
    kv_heads, span = logsum_ref.shape[1:]
    head_size = w_key.shape[1] // kv_heads
    scaling = 1.0 / math.sqrt(head_size)
    pieces = query_rows.shape[1]

    loads = [
        pltpu.make_async_copy(source, target, weight_sem.at[at])
        for at, (source, target) in enumerate(
            (
                (w_query_hbm, w_query),
                (w_key_hbm, w_key),
                (w_value_hbm, w_value),
                (w_attn_out_hbm, w_attn_out),
            )
        )
    ]

    def cache_loads(at):
        members = pl.ds(at * GROUP, GROUP)
        return (
            pltpu.make_async_copy(keys_hbm.at[members], keys.at[members], cache_sem.at[at, 0]),
            pltpu.make_async_copy(values_hbm.at[members], values.at[members], cache_sem.at[at, 1]),
        )

    for load in loads[:3]:
        load.start()
    for at in range(own_rows // GROUP):
        for load in cache_loads(at):
            load.start()
    loads[3].start()

    lane = lax.broadcasted_iota(jnp.int32, (1, extra_rows.shape[1]), 1)
    expert = lax.rem(lane, count)
    for b in range(own_rows):
        table = jnp.zeros(lane.shape, jnp.float32)
        for k in range(routes_ref.shape[0]):
            table = table + jnp.where(expert == routes_ref[k, b], route_weights_ref[k, b], 0.0)
        high = table.astype(jnp.bfloat16).astype(jnp.float32)
        middle = (table - high).astype(jnp.bfloat16).astype(jnp.float32)
        low = table - high - middle
        extra_rows[b : b + 1, :] = jnp.where(
            lane < count, high, jnp.where(lane < 2 * count, middle, low)
        )

    def normalise(widened, gain):
        mean = jnp.mean(widened * widened, axis=-1, keepdims=True)
        return (widened * lax.rsqrt(mean + EPSILON) * gain).astype(jnp.bfloat16)

    tokens = tokens_ref[...].astype(jnp.float32)
    normed = normalise(tokens, attn_gain_ref[...])
    wide_normed = normed.astype(jnp.float32)
    for head in range(kv_heads):
        row = w_forget_ref[pl.ds(head, 1), :].astype(jnp.float32)
        logit = jnp.sum(wide_normed * row, axis=1, keepdims=True) + forget_bias_ref[head]
        log_gate = jnp.minimum(logit, 0.0) - jnp.log1p(jnp.exp(-jnp.abs(logit)))
        gates[:, head, :] = jnp.broadcast_to(log_gate, (own_rows, gates.shape[2]))

    def project(weights):
        product = jnp.dot(normed, weights[...], preferred_element_type=jnp.float32)
        return product.astype(jnp.bfloat16).astype(jnp.float32)

    loads[0].wait()
    queries = project(w_query)
    for piece in range(pieces):
        query_rows[:, piece, :] = queries[:, piece * LANES : (piece + 1) * LANES]
    loads[1].wait()
    new_keys[...] = project(w_key)
    loads[2].wait()
    new_values[...] = project(w_value)

    piece_at = lax.broadcasted_iota(jnp.int32, (pieces, LANES), 0)
    lane_at = lax.broadcasted_iota(jnp.int32, (pieces, LANES), 1)
    in_place = (piece_at < pieces // kv_heads) == (lane_at < head_size)
    row_at = lax.rem(lax.broadcasted_iota(jnp.int32, (2 * pieces, span), 0), pieces)
    early = row_at < pieces // kv_heads
    position = lax.broadcasted_iota(jnp.int32, (2 * pieces, span), 1)
    head_position = lax.broadcasted_iota(jnp.int32, (kv_heads, span), 1)

    def sequence(b):
        valid = lengths_ref[b]
        plain = query_rows[b]
        turned = pltpu.roll(plain, head_size, 1)
        query = jnp.concatenate(
            [jnp.where(in_place, plain, 0.0), jnp.where(in_place, turned, 0.0)], axis=0
        )
        scores = lax.dot_general(
            query.astype(jnp.bfloat16),
            keys[b],
            (((1,), (1,)), ((), ())),
            preferred_element_type=jnp.float32,
        )
        logsum = logsum_ref[b]
        latest = jnp.sum(jnp.where(head_position == valid - 1, logsum, 0.0), axis=1, keepdims=True)
        offsets = (latest + gates[b][:, :1]) - logsum
        offset = jnp.where(early, offsets[0:1, :], offsets[1:2, :])
        scores = jnp.where(position < valid, scores * scaling + offset, -jnp.inf)
        own = jnp.sum(query * new_keys[pl.ds(b, 1), :], axis=1, keepdims=True) * scaling
        peak = jnp.maximum(jnp.max(scores, axis=1, keepdims=True), own)
        weight = jnp.exp(scores - peak)
        own_weight = jnp.exp(own - peak)
        inverse = 1.0 / (jnp.sum(weight, axis=1, keepdims=True) + own_weight)
        probs = (weight * inverse).astype(jnp.bfloat16)
        own_prob = (own_weight * inverse).astype(jnp.bfloat16).astype(jnp.float32)
        mixed = jnp.dot(probs, values[b], preferred_element_type=jnp.float32)
        mixed = mixed + own_prob * new_values[pl.ds(b, 1), :]
        first = jnp.where(in_place, mixed[:pieces], 0.0)
        other = jnp.where(in_place, mixed[pieces:], 0.0)
        return first + pltpu.roll(other, head_size, 1)

    def group(at, carried):
        for load in cache_loads(at):
            load.wait()
        results = [sequence(at * GROUP + member) for member in range(GROUP)]
        for member in range(GROUP):
            attended_rows[at * GROUP + member] = results[member]
        return carried

    lax.fori_loop(0, own_rows // GROUP, group, 0)

    attended = jnp.concatenate([attended_rows[:, piece, :] for piece in range(pieces)], axis=1)
    loads[3].wait()
    residual = tokens + jnp.dot(
        attended.astype(jnp.bfloat16), w_attn_out[...], preferred_element_type=jnp.float32
    )
    residual_ref[...] = residual
    block_ref[:, :width] = normalise(residual, ffn_gain_ref[...])
    block_ref[:, width:] = extra_rows[...].astype(jnp.bfloat16)


def attend(
    tokens,
    attn_gain,
    w_query,
    w_key,
    w_value,
    w_forget,
    forget_bias,
    w_attn_out,
    cache_keys,
    cache_values,
    cache_logsum,
    lengths,
    ffn_gain,
    routes,
    route_weights,
):
    count = lax.axis_size("ep")
    own_rows, width = tokens.shape
    kv_heads = cache_logsum.shape[1]
    pieces = w_query.shape[1] // LANES
    wide = width + -(-3 * count // LANES) * LANES
    bf16, f32 = jnp.bfloat16, jnp.float32
    near = pl.BlockSpec(memory_space=pltpu.VMEM)
    far = pl.BlockSpec(memory_space=pl.ANY)
    scalars = pl.BlockSpec(memory_space=pltpu.SMEM)
    return pl.pallas_call(
        lambda *refs: attend_kernel(count, *refs),
        out_shape=(
            jax.ShapeDtypeStruct((own_rows, width), f32),
            jax.ShapeDtypeStruct((own_rows, wide), bf16),
        ),
        in_specs=[near, near, far, far, far, near, scalars, far, far, far, near, scalars]
        + [near, scalars, scalars],
        out_specs=(near, near),
        scratch_shapes=[
            pltpu.VMEM(w_query.shape, bf16),
            pltpu.VMEM(w_key.shape, bf16),
            pltpu.VMEM(w_value.shape, bf16),
            pltpu.VMEM(w_attn_out.shape, bf16),
            pltpu.VMEM(cache_keys.shape, bf16),
            pltpu.VMEM(cache_values.shape, bf16),
            pltpu.VMEM((own_rows, pieces, LANES), f32),
            pltpu.VMEM((own_rows, w_key.shape[1]), f32),
            pltpu.VMEM((own_rows, w_value.shape[1]), f32),
            pltpu.VMEM((own_rows, kv_heads, LANES), f32),
            pltpu.VMEM((own_rows, pieces, LANES), f32),
            pltpu.VMEM((own_rows, wide - width), f32),
            pltpu.SemaphoreType.DMA((4,)),
            pltpu.SemaphoreType.DMA((own_rows // GROUP, 2)),
        ],
        compiler_params=pltpu.CompilerParams(vmem_limit_bytes=VMEM_BYTES),
        name="attend",
    )(
        tokens,
        attn_gain.reshape(1, -1),
        w_query,
        w_key,
        w_value,
        w_forget.T,
        forget_bias,
        w_attn_out,
        cache_keys,
        cache_values,
        cache_logsum,
        lengths,
        ffn_gain.reshape(1, -1),
        routes.T,
        route_weights.T,
    )


def body(
    tokens,
    attn_gain,
    w_query,
    w_key,
    w_value,
    w_forget,
    forget_bias,
    w_attn_out,
    cache_keys,
    cache_values,
    cache_logsum,
    lengths,
    ffn_gain,
    branch_gate,
    dense_gate,
    dense_up,
    dense_down,
    expert_gate,
    expert_up,
    expert_down,
    routes,
    route_weights,
):
    residual, block = attend(
        tokens,
        attn_gain,
        w_query,
        w_key,
        w_value,
        w_forget,
        forget_bias,
        w_attn_out,
        cache_keys,
        cache_values,
        cache_logsum,
        lengths,
        ffn_gain,
        routes,
        route_weights,
    )
    return exchange(
        block,
        residual,
        branch_gate,
        dense_gate,
        dense_up,
        dense_down,
        expert_gate,
        expert_up,
        expert_down,
    )


def solution(mesh):
    return jax.shard_map(
        body,
        mesh=mesh,
        in_specs=(
            P(("grp", "ep"), None),
            P(),
            P(),
            P(),
            P(),
            P(),
            P(),
            P(),
            P(("grp", "ep"), None, None),
            P(("grp", "ep"), None, None),
            P(("grp", "ep"), None, None),
            P(("grp", "ep")),
            P(),
            P(),
            P(None, "ep"),
            P(None, "ep"),
            P("ep", None),
            P("ep", None, None),
            P("ep", None, None),
            P("ep", None, None),
            P(("grp", "ep"), None),
            P(("grp", "ep"), None),
        ),
        out_specs=P(("grp", "ep"), None),
        check_vma=False,
    )
```
